32 devices in a mesh: kv: 8 (over z, x), tp: 4 (over y, core).
Axes of the slice: x: 2, y: 2, z: 4, core: 2. Of those that a mesh axis runs over, the one named last changes fastest.
Arguments:
- tokens: bfloat16 [128, 2048], P(None, 'kv'), may hold values from -16 to 16
- norm_gain: bfloat16 [2048], P('kv'), may hold values from 0.099609375 to 1.8984375
- w_query: bfloat16 [2048, 1024], P('kv', 'tp'), may hold values from -0.125 to 0.125
- w_key: bfloat16 [2048, 1024], P('kv', 'tp'), may hold values from -0.125 to 0.125
- w_value: bfloat16 [2048, 2048], P('kv', 'tp'), may hold values from -0.125 to 0.125
- w_gate: bfloat16 [2048, 2048], P('kv', 'tp'), may hold values from -0.125 to 0.125
- w_decay: bfloat16 [2048, 1024], P('kv', 'tp'), may hold values from -0.5 to 0.5
- log_decay: float32 [128, 1024], P('kv', 'tp'), may hold values from -1.5 to 0
- state: float32 [128, 8, 128, 256], P('kv', 'tp'), may hold values from -6 to 6
- out_gain: float32 [256], replicated, may hold values from 0.1 to 1.9
- w_out: bfloat16 [2048, 2048], P('tp', 'kv'), may hold values from -0.125 to 0.125
- mixer_gain: bfloat16 [2048], P('kv'), may hold values from 0.099609375 to 1.8984375
- w_ffgate: bfloat16 [2048, 6144], P('kv', 'tp'), may hold values from -0.125 to 0.125
- w_ffup: bfloat16 [2048, 6144], P('kv', 'tp'), may hold values from -0.125 to 0.125
- w_down: bfloat16 [6144, 2048], P('tp', 'kv'), may hold values from -0.078125 to 0.078125
Outputs:
- result: bfloat16 [128, 2048], P(None, 'kv')
- new_state: float32 [128, 8, 128, 256], P('kv', 'tp')
The draws below stay inside these ranges and needn't reach their ends.
All inputs are finite; a program needn't handle non-finite values.
Results may differ from the reference program's by a relative error of at most 0.028.
Values may be sent and summed in bfloat16 or wider, within the bound.
A program may use at most 64 MiB of HBM per device.

```python
import math
import jax
import jax.numpy as jnp
from jax import lax

D = 2048
HEADS = 8
DK = 128
DV = 256
FF = 6144
BATCH = 128
KW = 1024
VW = 2048
N_TP = 4


def draw_tokens(key, part):
    base = jnp.clip(jax.random.normal(jax.random.fold_in(key, 11), (BATCH, D), jnp.float32), -4.0, 4.0)
    rough = jax.random.uniform(jax.random.fold_in(key, 12), (1, D), jnp.float32, 0.5, 1.5)
    ramp = jnp.exp(jnp.linspace(0.0, math.log(6.0), D))[None, :]
    values = base * ramp * rough / 2.5
    return jnp.clip(values, -16.0, 16.0).astype(jnp.bfloat16)


def steps_of(key, shape, cuts, smallest, largest):
    def one(dim, shards_of):
        draws = jax.random.uniform(jax.random.fold_in(jax.random.fold_in(key, 6), dim), (shards_of,), jnp.float32, smallest / len(cuts), largest / len(cuts))
        return jnp.repeat(jnp.exp(draws), shape[dim] // shards_of).reshape((-1,) + (1,) * (len(shape) - dim - 1))

    loudness = one(*cuts[0])
    for cut in cuts[1:]:
        loudness = loudness * one(*cut)
    return loudness


def noise(own_key, dims, deviation, limit, shards=(), dtype=jnp.bfloat16):
    array = deviation * jax.random.normal(own_key, dims, jnp.float32)
    if shards:
        array = array * steps_of(own_key, dims, shards, -0.22, 0.18)
    return jnp.clip(array, -limit, limit).astype(dtype)


def setup_inputs(seed: int = 0) -> dict:
    arg_keys = jax.random.split(jax.random.key(seed), 16)
    tokens = draw_tokens(jax.random.fold_in(arg_keys[15], 71), 0)
    norm_gain = jnp.clip(1.0 + 0.18 * jax.random.normal(arg_keys[1], (D,), jnp.float32), 0.099609375, 1.8984375).astype(jnp.bfloat16)
    w_query = noise(arg_keys[2], (D, KW), D ** -0.5, 0.125, ((0, 8), (1, 4)))
    w_key = noise(arg_keys[3], (D, KW), D ** -0.5, 0.125, ((0, 8), (1, 4)))
    w_value = noise(arg_keys[4], (D, VW), D ** -0.5, 0.125, ((0, 8), (1, 4)))
    w_gate = noise(arg_keys[5], (D, VW), D ** -0.5, 0.125, ((0, 8), (1, 4)))
    w_decay = noise(arg_keys[6], (D, KW), (D // 16) ** -0.5, 0.5, ((0, 8), (1, 4)))
    log_decay = jnp.clip(-1.5 + 1.5 * jax.random.uniform(arg_keys[7], (BATCH, KW), jnp.float32) ** steps_of(arg_keys[7], (BATCH, KW), ((0, 8), (1, 4)), -0.2, 0.2), -1.5, 0.0)
    state = noise(arg_keys[8], (BATCH, HEADS, DK, DV), 1.0, 6.0, ((0, 8), (1, 4)), jnp.float32)
    out_gain = jnp.clip(1.0 + 0.18 * jax.random.normal(arg_keys[9], (DV,), jnp.float32), 0.1, 1.9)
    w_out = noise(arg_keys[10], (VW, D), VW ** -0.5, 0.125, ((0, 4), (1, 8)))
    mixer_gain = jnp.clip(1.0 + 0.18 * jax.random.normal(arg_keys[11], (D,), jnp.float32), 0.099609375, 1.8984375).astype(jnp.bfloat16)
    w_ffgate = noise(arg_keys[12], (D, FF), D ** -0.5, 0.125, ((0, 8), (1, 4)))
    w_ffup = noise(arg_keys[13], (D, FF), D ** -0.5, 0.125, ((0, 8), (1, 4)))
    w_down = noise(arg_keys[14], (FF, D), FF ** -0.5, 0.078125, ((0, 4), (1, 8)))
    return dict(tokens=tokens, norm_gain=norm_gain, w_query=w_query, w_key=w_key, w_value=w_value, w_gate=w_gate, w_decay=w_decay, log_decay=log_decay, state=state, out_gain=out_gain, w_out=w_out, mixer_gain=mixer_gain, w_ffgate=w_ffgate, w_ffup=w_ffup, w_down=w_down)


eps = 1e-06
gate_norm = 16.0

def group_sum(left, right, groups):
    width = left.shape[1] // groups
    total = jnp.zeros((left.shape[0], right.shape[1]), jnp.float32)
    for group in range(groups):
        part = jnp.dot(left[:, group * width:(group + 1) * width], right[group * width:(group + 1) * width], preferred_element_type=jnp.float32)
        part = lax.optimization_barrier(part.astype(jnp.bfloat16))
        total = total + part.astype(jnp.float32)
    return total

def reference(tokens, norm_gain, w_query, w_key, w_value, w_gate, w_decay, log_decay, state, out_gain, w_out, mixer_gain, w_ffgate, w_ffup, w_down):
    wide = tokens.astype(jnp.float32)
    scaled = (wide * norm_gain.astype(jnp.float32)).astype(jnp.bfloat16)
    inv = lax.rsqrt(lax.optimization_barrier(jnp.mean(wide * wide, axis=1, keepdims=True)) + eps)
    query = jnp.dot(scaled, w_query, preferred_element_type=jnp.float32) * inv
    key = jnp.dot(scaled, w_key, preferred_element_type=jnp.float32) * inv
    value = jnp.dot(scaled, w_value, preferred_element_type=jnp.float32) * inv
    gate = jnp.dot(scaled, w_gate, preferred_element_type=jnp.float32) * inv
    decay_pre = jnp.dot(scaled, w_decay, preferred_element_type=jnp.float32) * inv
    log_a = jax.nn.log_sigmoid(decay_pre) / gate_norm + log_decay
    query = query.reshape(BATCH, HEADS, DK) * DK ** (-0.5)
    key = key.reshape(BATCH, HEADS, DK)
    value = value.reshape(BATCH, HEADS, DV)
    new_state = state * jnp.exp(log_a).reshape(BATCH, HEADS, DK)[..., None] + key[..., None] * value[:, :, None, :]
    attended = jnp.einsum('bhk,bhkv->bhv', query, new_state, precision=lax.Precision.HIGHEST)
    normed = attended * lax.rsqrt(lax.optimization_barrier(jnp.mean(attended * attended, axis=2, keepdims=True)) + eps) * out_gain
    mixed = (normed.reshape(BATCH, VW) * jax.nn.silu(gate)).astype(jnp.bfloat16)
    attn_sum = group_sum(mixed, w_out, N_TP)
    middle = (wide + attn_sum).astype(jnp.bfloat16)
    wide2 = middle.astype(jnp.float32)
    scaled2 = (wide2 * mixer_gain.astype(jnp.float32)).astype(jnp.bfloat16)
    inv2 = lax.rsqrt(lax.optimization_barrier(jnp.mean(wide2 * wide2, axis=1, keepdims=True)) + eps)
    gate2 = jnp.dot(scaled2, w_ffgate, preferred_element_type=jnp.float32) * inv2
    upper = jnp.dot(scaled2, w_ffup, preferred_element_type=jnp.float32) * inv2
    hidden = (jax.nn.silu(gate2) * upper).astype(jnp.bfloat16)
    down_sum = group_sum(hidden, w_down, N_TP)
    result = (wide2 + down_sum).astype(jnp.bfloat16)
    return (result, new_state)
```

```python
import functools

import jax
import jax.numpy as jnp
from jax import lax
from jax.experimental import pallas as pl
from jax.experimental.pallas import tpu as pltpu
from jax.sharding import PartitionSpec as P

eps = 1e-06
gate_norm = 16.0
LANES = 128
F32 = jnp.float32
BF16 = jnp.bfloat16


def remote(src, dst, send_sem, recv_sem, device):
    return pltpu.make_async_remote_copy(
        src_ref=src,
        dst_ref=dst,
        send_sem=send_sem,
        recv_sem=recv_sem,
        device_id=device,
        device_id_type=pl.DeviceIdType.MESH,
    )


def split_axis(n_kv):
    n_in = 1
    while n_in * n_in * 4 <= n_kv:
        n_in *= 2
    return n_kv // n_in, n_in


def ff_chunks(width):
    tiles = max(width // LANES, 1)
    return max(n for n in (1, 2, 3, 4) if tiles % n == 0)


def kernel(
    n_kv,
    n_tp,
    d_model,
    tokens_ref,
    norm_gain_ref,
    wq_hbm,
    wk_hbm,
    wv_hbm,
    wg_hbm,
    wd_hbm,
    log_decay_ref,
    state_hbm,
    out_gain_ref,
    wo_hbm,
    mixer_gain_ref,
    wfg_hbm,
    wfu_hbm,
    wdn_hbm,
    result_ref,
    ns_ref,
    wq,
    wk,
    wv,
    wg,
    wd,
    wo,
    wfg,
    wfu,
    wdn,
    px,
    rx,
    pz,
    rz,
    att,
    mg,
    to,
    fx,
    frx,
    fz,
    frz,
    hg,
    td,
    middle_ref,
    load_sem,
    ax_s,
    ax_r,
    az_s,
    az_r,
    mz_s,
    mz_r,
    mx_s,
    mx_r,
    to_s,
    to_r,
    fx_s,
    fx_r,
    fz_s,
    fz_r,
    hz_s,
    hz_r,
    hx_s,
    hx_r,
    td_s,
    td_r,
):
    n_out, n_in = split_axis(n_kv)
    kv = lax.axis_index("kv")
    tp = lax.axis_index("tp")
    zi = kv // n_in
    xi = lax.rem(kv, n_in)
    rows = px.shape[2]
    batch = tokens_ref.shape[0]

    def x_peer(d):
        return lax.rem(xi + d, n_in)

    def z_peer(d):
        return lax.rem(zi + d, n_out)

    def z_back(d):
        return lax.rem(zi + n_out - d, n_out)

    def x_back(d):
        return lax.rem(xi + n_in - d, n_in)

    def x_dev(d):
        return (zi * n_in + x_peer(d), tp)

    def z_dev(d):
        return (z_peer(d) * n_in + xi, tp)

    def t_dev(d):
        return (kv, lax.rem(tp + d, n_tp))

    barrier = pltpu.get_barrier_semaphore()
    peers = (
        [x_dev(d) for d in range(1, n_in)]
        + [z_dev(d) for d in range(1, n_out)]
        + [t_dev(d) for d in range(1, n_tp)]
    )
    for dev in peers:
        pl.semaphore_signal(barrier, inc=1, device_id=dev, device_id_type=pl.DeviceIdType.MESH)

    loads = [
        pltpu.make_async_copy(src, dst, load_sem.at[i])
        for i, (src, dst) in enumerate(
            (
                (wq_hbm, wq),
                (wk_hbm, wk),
                (wd_hbm, wd),
                (wv_hbm, wv),
                (wg_hbm, wg),
                (state_hbm, ns_ref),
                (wo_hbm, wo),
                (wfg_hbm, wfg),
                (wfu_hbm, wfu),
                (wdn_hbm, wdn),
            )
        )
    ]
    for load in loads:
        load.start()
    load_q, load_k, load_d, load_v, load_g, load_state, load_o, load_fg, load_fu, load_dn = loads

    pending = []

    def launch(copy):
        copy.start()
        pending.append(copy)

    def scatter_rows(dst, value, lo):
        width = value.shape[1]
        value = value.astype(BF16)
        for z in range(n_out):
            for x in range(n_in):
                at = (z * n_in + x) * rows
                dst[x, z, :, lo : lo + width] = value[at : at + rows]

    def send_x(src, dst, s, r, c, lo, hi):
        cols = slice(lo, hi)
        return [
            remote(
                src.at[x_peer(d), :, :, cols],
                dst.at[d - 1, :, :, cols],
                s.at[c, d - 1],
                r.at[c, d - 1],
                x_dev(d),
            )
            for d in range(1, n_in)
        ]

    def send_z(src, dst, s, r, c, lo, hi):
        cols = slice(lo, hi)
        return [
            remote(
                src.at[z_peer(d), :, cols],
                dst.at[d - 1, :, cols],
                s.at[c, d - 1],
                r.at[c, d - 1],
                z_dev(d),
            )
            for d in range(1, n_out)
        ]

    def reduce_x(src, got, dst, copies, lo, hi):
        for copy in copies:
            copy.wait_recv()
        total = src[xi, :, :, lo:hi].astype(F32)
        for d in range(1, n_in):
            total = total + got[d - 1, :, :, lo:hi].astype(F32)
        dst[:, :, lo:hi] = total.astype(BF16)

    def reduce_z(src, got, copies, lo, hi):
        for copy in copies:
            copy.wait_recv()
        total = src[zi, :, lo:hi].astype(F32)
        for d in range(1, n_out):
            total = total + got[d - 1, :, lo:hi].astype(F32)
        return total

    wide = tokens_ref[...].astype(F32)
    scaled = (wide * norm_gain_ref[...].astype(F32).reshape(1, -1)).astype(BF16)
    squares = jnp.broadcast_to(jnp.sum(wide * wide, axis=1, keepdims=True), (batch, LANES))

    kw = wq.shape[1]
    vw = wv.shape[1]
    q_at = LANES
    k_at = q_at + kw
    d_at = k_at + kw
    v_at = d_at + kw
    g_at = v_at + vw
    end = g_at + vw
    bounds = ((0, d_at), (d_at, g_at), (g_at, end))
    parts = (
        ((wq, load_q, q_at), (wk, load_k, k_at)),
        ((wd, load_d, d_at), (wv, load_v, v_at)),
        ((wg, load_g, g_at),),
    )
    x_copies = []
    for c, ((lo, hi), part) in enumerate(zip(bounds, parts)):
        if c == 0:
            scatter_rows(px, squares, 0)
        for weight, load, at in part:
            load.wait()
            scatter_rows(px, jnp.dot(scaled, weight[...], preferred_element_type=F32), at)
        if c == 0:
            pl.semaphore_wait(barrier, len(peers))
        copies = send_x(px, rx, ax_s, ax_r, c, lo, hi)
        for copy in copies:
            launch(copy)
        x_copies.append(copies)
    z_copies = []
    for c, (lo, hi) in enumerate(bounds):
        reduce_x(px, rx, pz, x_copies[c], lo, hi)
        copies = send_z(pz, rz, az_s, az_r, c, lo, hi)
        for copy in copies:
            launch(copy)
        z_copies.append(copies)

    first = reduce_z(pz, rz, z_copies[0], *bounds[0])
    inv = lax.rsqrt(first[:, :1] / d_model + eps)
    second = reduce_z(pz, rz, z_copies[1], *bounds[1])

    heads, dk, dv = ns_ref.shape[1:]
    query = first[:, q_at : q_at + kw] * inv * dk ** (-0.5)
    keys = first[:, k_at : k_at + kw] * inv
    pre = second[:, :kw] * inv
    values = second[:, kw:] * inv
    log_sig = jnp.minimum(pre, 0.0) - jnp.log1p(jnp.exp(-jnp.abs(pre)))
    decay = jnp.exp(log_sig / gate_norm + log_decay_ref[...])
    load_state.wait()
    for h in range(heads):
        ks = slice(h * dk, (h + 1) * dk)
        q_t = query[:, ks].T
        k_t = keys[:, ks].T
        a_t = decay[:, ks].T
        for b in range(rows):
            col = slice(b, b + 1)
            v_row = values[b : b + 1, h * dv : (h + 1) * dv]
            new = ns_ref[b, h] * a_t[:, col] + k_t[:, col] * v_row
            ns_ref[b, h] = new
            att[h, b : b + 1, :] = jnp.sum(new * q_t[:, col], axis=0, keepdims=True)

    gate = reduce_z(pz, rz, z_copies[2], *bounds[2]) * inv
    for h in range(heads):
        got = att[h]
        normed = (
            got
            * lax.rsqrt(jnp.mean(got * got, axis=1, keepdims=True) + eps)
            * out_gain_ref[...]
        )
        cols = slice(h * dv, (h + 1) * dv)
        mg[zi, xi, :, cols] = (normed * jax.nn.silu(gate[:, cols])).astype(BF16)

    def gather_z(buf, s, r):
        for d in range(1, n_out):
            launch(remote(buf.at[zi, xi], buf.at[zi, xi], s.at[d - 1], r.at[d - 1], z_dev(d)))

    def forward_x(buf, zs, zr, s, r):
        for dz in range(n_out):
            slot = buf.at[z_back(dz), xi]
            if dz:
                remote(slot, slot, zs.at[dz - 1], zr.at[dz - 1], z_dev(dz)).wait_recv()
            for d in range(1, n_in):
                launch(remote(slot, slot, s.at[dz, d - 1], r.at[dz, d - 1], x_dev(d)))

    def arrive_x(buf, s, r):
        for dz in range(n_out):
            for d in range(1, n_in):
                slot = buf.at[z_back(dz), x_back(d)]
                remote(slot, slot, s.at[dz, d - 1], r.at[dz, d - 1], x_dev(d)).wait_recv()

    gather_z(mg, mz_s, mz_r)
    forward_x(mg, mz_s, mz_r, mx_s, mx_r)
    load_o.wait()
    arrive_x(mg, mx_s, mx_r)

    def sum_groups(buf, s, r):
        for d in range(1, n_tp):
            launch(remote(buf.at[tp], buf.at[tp], s.at[d - 1], r.at[d - 1], t_dev(d)))
        for d in range(1, n_tp):
            slot = buf.at[lax.rem(tp + n_tp - d, n_tp)]
            remote(slot, slot, s.at[d - 1], r.at[d - 1], t_dev(d)).wait_recv()
        total = buf[0].astype(F32)
        for g in range(1, n_tp):
            total = total + buf[g].astype(F32)
        return total

    mixed = mg[...].reshape(batch, vw)
    to[tp] = jnp.dot(mixed, wo[...], preferred_element_type=F32).astype(BF16)
    middle = (tokens_ref[...].astype(F32) + sum_groups(to, to_s, to_r)).astype(BF16)
    middle_ref[...] = middle

    wide2 = middle.astype(F32)
    scaled2 = (wide2 * mixer_gain_ref[...].astype(F32).reshape(1, -1)).astype(BF16)
    squares2 = jnp.broadcast_to(jnp.sum(wide2 * wide2, axis=1, keepdims=True), (batch, LANES))
    ff = wfg.shape[1]
    n_c = ff_chunks(ff)
    fc = ff // n_c
    fbounds = [
        (0 if c == 0 else LANES + 2 * fc * c, LANES + 2 * fc * (c + 1)) for c in range(n_c)
    ]
    load_fg.wait()
    load_fu.wait()
    fx_copies = []
    for c, (lo, hi) in enumerate(fbounds):
        if c == 0:
            scatter_rows(fx, squares2, 0)
        cols = slice(c * fc, (c + 1) * fc)
        at = LANES + 2 * fc * c
        scatter_rows(fx, jnp.dot(scaled2, wfg[:, cols], preferred_element_type=F32), at)
        scatter_rows(fx, jnp.dot(scaled2, wfu[:, cols], preferred_element_type=F32), at + fc)
        copies = send_x(fx, frx, fx_s, fx_r, c, lo, hi)
        for copy in copies:
            launch(copy)
        fx_copies.append(copies)

    fz_copies = [None] * n_c
    inv2 = [None]

    def to_z(c):
        lo, hi = fbounds[c]
        reduce_x(fx, frx, fz, fx_copies[c], lo, hi)
        fz_copies[c] = send_z(fz, frz, fz_s, fz_r, c, lo, hi)
        for copy in fz_copies[c]:
            launch(copy)

    def activate(c):
        terms = reduce_z(fz, frz, fz_copies[c], *fbounds[c])
        if c == 0:
            inv2[0] = lax.rsqrt(terms[:, :1] / d_model + eps)
            terms = terms[:, LANES:]
        terms = terms * inv2[0]
        hg[c, zi, xi] = (jax.nn.silu(terms[:, :fc]) * terms[:, fc:]).astype(BF16)
        gather_z(hg.at[c], hz_s.at[c], hz_r.at[c])

    def hand_on(c):
        forward_x(hg.at[c], hz_s.at[c], hz_r.at[c], hx_s.at[c], hx_r.at[c])

    for t in range(n_c + 3):
        if t < n_c:
            to_z(t)
        if 0 <= t - 2 < n_c:
            activate(t - 2)
        if 0 <= t - 3 < n_c:
            hand_on(t - 3)

    load_dn.wait()
    down = None
    for c in range(n_c):
        arrive_x(hg.at[c], hx_s.at[c], hx_r.at[c])
        term = jnp.dot(
            hg[c].reshape(batch, fc),
            wdn[c * fc : (c + 1) * fc, :],
            preferred_element_type=F32,
        )
        down = term if down is None else down + term
    td[tp] = down.astype(BF16)
    total = sum_groups(td, td_s, td_r)
    result_ref[...] = (middle_ref[...].astype(F32) + total).astype(BF16)

    for copy in pending:
        copy.wait_send()


def body(n_kv, n_tp, *args):
    (
        tokens,
        norm_gain,
        w_query,
        w_key,
        w_value,
        w_gate,
        w_decay,
        log_decay,
        state,
        out_gain,
        w_out,
        mixer_gain,
        w_ffgate,
        w_ffup,
        w_down,
    ) = args
    n_out, n_in = split_axis(n_kv)
    batch, feats = tokens.shape
    rows, heads, dk, dv = state.shape
    kw = w_query.shape[1]
    vw = w_value.shape[1]
    ff = w_ffgate.shape[1]
    n_c = ff_chunks(ff)
    fc = ff // n_c
    width = LANES + 3 * kw + 2 * vw
    fwidth = LANES + 2 * ff
    m_in, m_out, m_tp = max(n_in - 1, 1), max(n_out - 1, 1), max(n_tp - 1, 1)
    dma = pltpu.SemaphoreType.DMA
    vmem = pltpu.VMEM
    whole = pl.BlockSpec(memory_space=pltpu.VMEM)
    far = pl.BlockSpec(memory_space=pl.ANY)
    sems = [
        (10,),
        (3, m_in),
        (3, m_in),
        (3, m_out),
        (3, m_out),
        (m_out,),
        (m_out,),
        (n_out, m_in),
        (n_out, m_in),
        (m_tp,),
        (m_tp,),
        (n_c, m_in),
        (n_c, m_in),
        (n_c, m_out),
        (n_c, m_out),
        (n_c, m_out),
        (n_c, m_out),
        (n_c, n_out, m_in),
        (n_c, n_out, m_in),
        (m_tp,),
        (m_tp,),
    ]
    result, new_state = pl.pallas_call(
        functools.partial(kernel, n_kv, n_tp, feats * n_kv),
        out_shape=(
            vmem((batch, feats), BF16),
            vmem(state.shape, F32),
        ),
        in_specs=[
            whole,
            whole,
            far,
            far,
            far,
            far,
            far,
            whole,
            far,
            whole,
            far,
            whole,
            far,
            far,
            far,
        ],
        out_specs=(whole, whole),
        scratch_shapes=[
            vmem(w_query.shape, BF16),
            vmem(w_key.shape, BF16),
            vmem(w_value.shape, BF16),
            vmem(w_gate.shape, BF16),
            vmem(w_decay.shape, BF16),
            vmem(w_out.shape, BF16),
            vmem(w_ffgate.shape, BF16),
            vmem(w_ffup.shape, BF16),
            vmem(w_down.shape, BF16),
            vmem((n_in, n_out, rows, width), BF16),
            vmem((m_in, n_out, rows, width), BF16),
            vmem((n_out, rows, width), BF16),
            vmem((m_out, rows, width), BF16),
            vmem((heads, rows, dv), F32),
            vmem((n_out, n_in, rows, vw), BF16),
            vmem((n_tp, batch, feats), BF16),
            vmem((n_in, n_out, rows, fwidth), BF16),
            vmem((m_in, n_out, rows, fwidth), BF16),
            vmem((n_out, rows, fwidth), BF16),
            vmem((m_out, rows, fwidth), BF16),
            vmem((n_c, n_out, n_in, rows, fc), BF16),
            vmem((n_tp, batch, feats), BF16),
            vmem((batch, feats), BF16),
        ]
        + [dma(shape) for shape in sems],
        compiler_params=pltpu.CompilerParams(
            collective_id=0, has_side_effects=True, vmem_limit_bytes=56 * 2**20
        ),
    )(
        tokens,
        norm_gain,
        w_query,
        w_key,
        w_value,
        w_gate,
        w_decay,
        log_decay,
        state,
        out_gain.reshape(1, dv),
        w_out,
        mixer_gain,
        w_ffgate,
        w_ffup,
        w_down,
    )
    return (result, new_state)


def solution(mesh):
    return jax.shard_map(
        functools.partial(body, mesh.shape["kv"], mesh.shape["tp"]),
        mesh=mesh,
        in_specs=(
            P(None, "kv"),
            P("kv"),
            P("kv", "tp"),
            P("kv", "tp"),
            P("kv", "tp"),
            P("kv", "tp"),
            P("kv", "tp"),
            P("kv", "tp"),
            P("kv", "tp", None, None),
            P(),
            P("tp", "kv"),
            P("kv"),
            P("kv", "tp"),
            P("kv", "tp"),
            P("tp", "kv"),
        ),
        out_specs=(P(None, "kv"), P("kv", "tp", None, None)),
        check_vma=False,
    )
```

```python
import functools

import jax
import jax.numpy as jnp
from jax import lax
from jax.experimental import pallas as pl
from jax.experimental.pallas import tpu as pltpu
from jax.sharding import PartitionSpec as P

eps = 1e-06
gate_norm = 16.0
LANES = 128
CHUNKS = 6
LAG_Z = 6
LAG_X = 8
F32 = jnp.float32
BF16 = jnp.bfloat16


def remote(src, dst, send_sem, recv_sem, device):
    return pltpu.make_async_remote_copy(
        src_ref=src,
        dst_ref=dst,
        send_sem=send_sem,
        recv_sem=recv_sem,
        device_id=device,
        device_id_type=pl.DeviceIdType.MESH,
    )


def split_axis(n_kv):
    n_in = 1
    while n_in * n_in * 4 <= n_kv:
        n_in *= 2
    return n_kv // n_in, n_in


def ff_chunks(width):
    if width % LANES:
        return [(0, width)]
    left, at, ranges = width // LANES, 0, []
    while left:
        take = min(left, -(-(width // LANES) // CHUNKS))
        ranges.append((at, at + take * LANES))
        at += take * LANES
        left -= take
    return ranges


def kernel(
    n_kv,
    n_tp,
    d_model,
    tokens_ref,
    norm_gain_ref,
    wq_hbm,
    wk_hbm,
    wv_hbm,
    wg_hbm,
    wd_hbm,
    log_decay_ref,
    state_hbm,
    out_gain_ref,
    wo_hbm,
    mixer_gain_ref,
    wfg_hbm,
    wfu_hbm,
    wdn_hbm,
    result_ref,
    ns_ref,
    wq,
    wk,
    wv,
    wg,
    wd,
    wo,
    wfg,
    wfu,
    wdn,
    px,
    rx,
    pz,
    rz,
    att,
    mg,
    to,
    fx,
    frx,
    fz,
    frz,
    hg,
    td,
    middle_ref,
    load_sem,
    ax_s,
    ax_r,
    az_s,
    az_r,
    mz_s,
    mz_r,
    mx_s,
    mx_r,
    to_s,
    to_r,
    fx_s,
    fx_r,
    fz_s,
    fz_r,
    hz_s,
    hz_r,
    hx_s,
    hx_r,
    td_s,
    td_r,
):
    n_out, n_in = split_axis(n_kv)
    kv = lax.axis_index("kv")
    tp = lax.axis_index("tp")
    zi = kv // n_in
    xi = lax.rem(kv, n_in)
    rows = px.shape[2]
    batch = tokens_ref.shape[0]

    def x_peer(d):
        return lax.rem(xi + d, n_in)

    def z_peer(d):
        return lax.rem(zi + d, n_out)

    def z_back(d):
        return lax.rem(zi + n_out - d, n_out)

    def x_back(d):
        return lax.rem(xi + n_in - d, n_in)

    def x_dev(d):
        return (zi * n_in + x_peer(d), tp)

    def z_dev(d):
        return (z_peer(d) * n_in + xi, tp)

    def t_dev(d):
        return (kv, lax.rem(tp + d, n_tp))

    barrier = pltpu.get_barrier_semaphore()
    peers = (
        [x_dev(d) for d in range(1, n_in)]
        + [z_dev(d) for d in range(1, n_out)]
        + [t_dev(d) for d in range(1, n_tp)]
    )
    for dev in peers:
        pl.semaphore_signal(barrier, inc=1, device_id=dev, device_id_type=pl.DeviceIdType.MESH)

    loads = [
        pltpu.make_async_copy(src, dst, load_sem.at[i])
        for i, (src, dst) in enumerate(
            (
                (wq_hbm, wq),
                (wk_hbm, wk),
                (wd_hbm, wd),
                (wv_hbm, wv),
                (wg_hbm, wg),
                (state_hbm, ns_ref),
                (wo_hbm, wo),
                (wfg_hbm, wfg),
                (wfu_hbm, wfu),
                (wdn_hbm, wdn),
            )
        )
    ]
    for load in loads[:5]:
        load.start()
    load_q, load_k, load_d, load_v, load_g, load_state, load_o, load_fg, load_fu, load_dn = loads

    pending = []

    def launch(copy):
        copy.start()
        pending.append(copy)

    def scatter_rows(dst, value, lo):
        width = value.shape[1]
        value = value.astype(BF16)
        for z in range(n_out):
            for x in range(n_in):
                at = (z * n_in + x) * rows
                dst[x, z, :, lo : lo + width] = value[at : at + rows]

    def send_x(src, dst, s, r, c, lo, hi):
        cols = slice(lo, hi)
        return [
            remote(
                src.at[x_peer(d), :, :, cols],
                dst.at[d - 1, :, :, cols],
                s.at[c, d - 1],
                r.at[c, d - 1],
                x_dev(d),
            )
            for d in range(1, n_in)
        ]

    def send_z(src, dst, s, r, c, lo, hi):
        cols = slice(lo, hi)
        return [
            remote(
                src.at[z_peer(d), :, cols],
                dst.at[d - 1, :, cols],
                s.at[c, d - 1],
                r.at[c, d - 1],
                z_dev(d),
            )
            for d in range(1, n_out)
        ]

    def reduce_x(src, got, dst, copies, lo, hi):
        for copy in copies:
            copy.wait_recv()
        total = src[xi, :, :, lo:hi].astype(F32)
        for d in range(1, n_in):
            total = total + got[d - 1, :, :, lo:hi].astype(F32)
        dst[:, :, lo:hi] = total.astype(BF16)

    def reduce_z(src, got, copies, lo, hi):
        for copy in copies:
            copy.wait_recv()
        total = src[zi, :, lo:hi].astype(F32)
        for d in range(1, n_out):
            total = total + got[d - 1, :, lo:hi].astype(F32)
        return total

    wide = tokens_ref[...].astype(F32)
    scaled = (wide * norm_gain_ref[...].astype(F32).reshape(1, -1)).astype(BF16)
    squares = jnp.broadcast_to(jnp.sum(wide * wide, axis=1, keepdims=True), (batch, LANES))

    kw = wq.shape[1]
    vw = wv.shape[1]
    q_at = LANES
    k_at = q_at + kw
    d_at = k_at + kw
    v_at = d_at + kw
    g_at = v_at + vw
    end = g_at + vw
    bounds = ((0, d_at), (d_at, g_at), (g_at, end))
    parts = (
        ((wq, load_q, q_at), (wk, load_k, k_at)),
        ((wd, load_d, d_at), (wv, load_v, v_at)),
        ((wg, load_g, g_at),),
    )
    x_copies = []
    for c, ((lo, hi), part) in enumerate(zip(bounds, parts)):
        if c == 0:
            scatter_rows(px, squares, 0)
        for weight, load, at in part:
            load.wait()
            scatter_rows(px, jnp.dot(scaled, weight[...], preferred_element_type=F32), at)
        if c == 0:
            pl.semaphore_wait(barrier, len(peers))
        copies = send_x(px, rx, ax_s, ax_r, c, lo, hi)
        for copy in copies:
            launch(copy)
        x_copies.append(copies)
    for load in loads[5:]:
        load.start()
    z_copies = []
    for c, (lo, hi) in enumerate(bounds):
        reduce_x(px, rx, pz, x_copies[c], lo, hi)
        copies = send_z(pz, rz, az_s, az_r, c, lo, hi)
        for copy in copies:
            launch(copy)
        z_copies.append(copies)

    first = reduce_z(pz, rz, z_copies[0], *bounds[0])
    inv = lax.rsqrt(first[:, :1] / d_model + eps)
    second = reduce_z(pz, rz, z_copies[1], *bounds[1])

    heads, dk, dv = ns_ref.shape[1:]
    query = first[:, q_at : q_at + kw] * inv * dk ** (-0.5)
    keys = first[:, k_at : k_at + kw] * inv
    pre = second[:, :kw] * inv
    values = second[:, kw:] * inv
    log_sig = jnp.minimum(pre, 0.0) - jnp.log1p(jnp.exp(-jnp.abs(pre)))
    decay = jnp.exp(log_sig / gate_norm + log_decay_ref[...])
    load_state.wait()
    for h in range(heads):
        ks = slice(h * dk, (h + 1) * dk)
        q_t = query[:, ks].T
        k_t = keys[:, ks].T
        a_t = decay[:, ks].T
        for b in range(rows):
            col = slice(b, b + 1)
            v_row = values[b : b + 1, h * dv : (h + 1) * dv]
            new = ns_ref[b, h] * a_t[:, col] + k_t[:, col] * v_row
            ns_ref[b, h] = new
            att[h, b : b + 1, :] = jnp.sum(new * q_t[:, col], axis=0, keepdims=True)

    gate = reduce_z(pz, rz, z_copies[2], *bounds[2]) * inv
    for h in range(heads):
        got = att[h]
        normed = (
            got
            * lax.rsqrt(jnp.mean(got * got, axis=1, keepdims=True) + eps)
            * out_gain_ref[...]
        )
        cols = slice(h * dv, (h + 1) * dv)
        mg[zi, xi, :, cols] = (normed * jax.nn.silu(gate[:, cols])).astype(BF16)

    def gather_z(buf, cols, s, r):
        for d in range(1, n_out):
            own = buf.at[zi, xi, :, cols]
            launch(remote(own, own, s.at[d - 1], r.at[d - 1], z_dev(d)))

    def forward_x(buf, cols, zs, zr, s, r):
        for dz in range(n_out):
            slot = buf.at[z_back(dz), xi, :, cols]
            if dz:
                remote(slot, slot, zs.at[dz - 1], zr.at[dz - 1], z_dev(dz)).wait_recv()
            for d in range(1, n_in):
                launch(remote(slot, slot, s.at[dz, d - 1], r.at[dz, d - 1], x_dev(d)))

    def arrive_x(buf, cols, s, r):
        for dz in range(n_out):
            for d in range(1, n_in):
                slot = buf.at[z_back(dz), x_back(d), :, cols]
                remote(slot, slot, s.at[dz, d - 1], r.at[dz, d - 1], x_dev(d)).wait_recv()

    gather_z(mg, slice(0, vw), mz_s, mz_r)
    forward_x(mg, slice(0, vw), mz_s, mz_r, mx_s, mx_r)
    load_o.wait()
    arrive_x(mg, slice(0, vw), mx_s, mx_r)

    def sum_groups(buf, s, r):
        for d in range(1, n_tp):
            launch(remote(buf.at[tp], buf.at[tp], s.at[d - 1], r.at[d - 1], t_dev(d)))
        for d in range(1, n_tp):
            slot = buf.at[lax.rem(tp + n_tp - d, n_tp)]
            remote(slot, slot, s.at[d - 1], r.at[d - 1], t_dev(d)).wait_recv()
        total = buf[0].astype(F32)
        for g in range(1, n_tp):
            total = total + buf[g].astype(F32)
        return total

    mixed = mg[...].reshape(batch, vw)
    to[tp] = jnp.dot(mixed, wo[...], preferred_element_type=F32).astype(BF16)
    middle = (tokens_ref[...].astype(F32) + sum_groups(to, to_s, to_r)).astype(BF16)
    middle_ref[...] = middle

    wide2 = middle.astype(F32)
    scaled2 = (wide2 * mixer_gain_ref[...].astype(F32).reshape(1, -1)).astype(BF16)
    squares2 = jnp.broadcast_to(jnp.sum(wide2 * wide2, axis=1, keepdims=True), (batch, LANES))
    ff = wfg.shape[1]
    chunks = ff_chunks(ff)
    n_c = len(chunks)
    fbounds = [(LANES + 2 * lo if lo else 0, LANES + 2 * hi) for lo, hi in chunks]
    load_fg.wait()
    load_fu.wait()
    fx_copies = []
    for c, (lo, hi) in enumerate(fbounds):
        if c == 0:
            scatter_rows(fx, squares2, 0)
        cols = slice(*chunks[c])
        fc = chunks[c][1] - chunks[c][0]
        at = hi - 2 * fc
        scatter_rows(fx, jnp.dot(scaled2, wfg[:, cols], preferred_element_type=F32), at)
        scatter_rows(fx, jnp.dot(scaled2, wfu[:, cols], preferred_element_type=F32), at + fc)
        copies = send_x(fx, frx, fx_s, fx_r, c, lo, hi)
        for copy in copies:
            launch(copy)
        fx_copies.append(copies)

    fz_copies = [None] * n_c
    inv2 = [None]

    def to_z(c):
        lo, hi = fbounds[c]
        reduce_x(fx, frx, fz, fx_copies[c], lo, hi)
        fz_copies[c] = send_z(fz, frz, fz_s, fz_r, c, lo, hi)
        for copy in fz_copies[c]:
            launch(copy)

    def activate(c):
        terms = reduce_z(fz, frz, fz_copies[c], *fbounds[c])
        if c == 0:
            inv2[0] = lax.rsqrt(terms[:, :1] / d_model + eps)
            terms = terms[:, LANES:]
        terms = terms * inv2[0]
        fc = terms.shape[1] // 2
        cols = slice(*chunks[c])
        hg[zi, xi, :, cols] = (jax.nn.silu(terms[:, :fc]) * terms[:, fc:]).astype(BF16)
        gather_z(hg, cols, hz_s.at[c], hz_r.at[c])

    def hand_on(c):
        forward_x(hg, slice(*chunks[c]), hz_s.at[c], hz_r.at[c], hx_s.at[c], hx_r.at[c])

    for t in range(n_c + LAG_X):
        if t < n_c:
            to_z(t)
        if 0 <= t - LAG_Z < n_c:
            activate(t - LAG_Z)
        if 0 <= t - LAG_X < n_c:
            hand_on(t - LAG_X)

    load_dn.wait()
    down = None
    for c, (lo, hi) in enumerate(chunks):
        arrive_x(hg, slice(*chunks[c]), hx_s.at[c], hx_r.at[c])
        term = jnp.dot(
            hg[:, :, :, lo:hi].reshape(batch, hi - lo),
            wdn[lo:hi, :],
            preferred_element_type=F32,
        )
        down = term if down is None else down + term
    td[tp] = down.astype(BF16)
    total = sum_groups(td, td_s, td_r)
    result_ref[...] = (middle_ref[...].astype(F32) + total).astype(BF16)

    for copy in pending:
        copy.wait_send()


def body(n_kv, n_tp, *args):
    (
        tokens,
        norm_gain,
        w_query,
        w_key,
        w_value,
        w_gate,
        w_decay,
        log_decay,
        state,
        out_gain,
        w_out,
        mixer_gain,
        w_ffgate,
        w_ffup,
        w_down,
    ) = args
    n_out, n_in = split_axis(n_kv)
    batch, feats = tokens.shape
    rows, heads, dk, dv = state.shape
    kw = w_query.shape[1]
    vw = w_value.shape[1]
    ff = w_ffgate.shape[1]
    n_c = len(ff_chunks(ff))
    width = LANES + 3 * kw + 2 * vw
    fwidth = LANES + 2 * ff
    m_in, m_out, m_tp = max(n_in - 1, 1), max(n_out - 1, 1), max(n_tp - 1, 1)
    dma = pltpu.SemaphoreType.DMA
    vmem = pltpu.VMEM
    whole = pl.BlockSpec(memory_space=pltpu.VMEM)
    far = pl.BlockSpec(memory_space=pl.ANY)
    sems = [
        (10,),
        (3, m_in),
        (3, m_in),
        (3, m_out),
        (3, m_out),
        (m_out,),
        (m_out,),
        (n_out, m_in),
        (n_out, m_in),
        (m_tp,),
        (m_tp,),
        (n_c, m_in),
        (n_c, m_in),
        (n_c, m_out),
        (n_c, m_out),
        (n_c, m_out),
        (n_c, m_out),
        (n_c, n_out, m_in),
        (n_c, n_out, m_in),
        (m_tp,),
        (m_tp,),
    ]
    result, new_state = pl.pallas_call(
        functools.partial(kernel, n_kv, n_tp, feats * n_kv),
        out_shape=(
            vmem((batch, feats), BF16),
            vmem(state.shape, F32),
        ),
        in_specs=[
            whole,
            whole,
            far,
            far,
            far,
            far,
            far,
            whole,
            far,
            whole,
            far,
            whole,
            far,
            far,
            far,
        ],
        out_specs=(whole, whole),
        scratch_shapes=[
            vmem(w_query.shape, BF16),
            vmem(w_key.shape, BF16),
            vmem(w_value.shape, BF16),
            vmem(w_gate.shape, BF16),
            vmem(w_decay.shape, BF16),
            vmem(w_out.shape, BF16),
            vmem(w_ffgate.shape, BF16),
            vmem(w_ffup.shape, BF16),
            vmem(w_down.shape, BF16),
            vmem((n_in, n_out, rows, width), BF16),
            vmem((m_in, n_out, rows, width), BF16),
            vmem((n_out, rows, width), BF16),
            vmem((m_out, rows, width), BF16),
            vmem((heads, rows, dv), F32),
            vmem((n_out, n_in, rows, vw), BF16),
            vmem((n_tp, batch, feats), BF16),
            vmem((n_in, n_out, rows, fwidth), BF16),
            vmem((m_in, n_out, rows, fwidth), BF16),
            vmem((n_out, rows, fwidth), BF16),
            vmem((m_out, rows, fwidth), BF16),
            vmem((n_out, n_in, rows, ff), BF16),
            vmem((n_tp, batch, feats), BF16),
            vmem((batch, feats), BF16),
        ]
        + [dma(shape) for shape in sems],
        compiler_params=pltpu.CompilerParams(
            collective_id=0, has_side_effects=True, vmem_limit_bytes=56 * 2**20
        ),
    )(
        tokens,
        norm_gain,
        w_query,
        w_key,
        w_value,
        w_gate,
        w_decay,
        log_decay,
        state,
        out_gain.reshape(1, dv),
        w_out,
        mixer_gain,
        w_ffgate,
        w_ffup,
        w_down,
    )
    return (result, new_state)


def solution(mesh):
    return jax.shard_map(
        functools.partial(body, mesh.shape["kv"], mesh.shape["tp"]),
        mesh=mesh,
        in_specs=(
            P(None, "kv"),
            P("kv"),
            P("kv", "tp"),
            P("kv", "tp"),
            P("kv", "tp"),
            P("kv", "tp"),
            P("kv", "tp"),
            P("kv", "tp"),
            P("kv", "tp", None, None),
            P(),
            P("tp", "kv"),
            P("kv"),
            P("kv", "tp"),
            P("kv", "tp"),
            P("tp", "kv"),
        ),
        out_specs=(P(None, "kv"), P("kv", "tp", None, None)),
        check_vma=False,
    )
```
